32 devices in a mesh: ep: 8 (over z, y), tp: 4 (over x, core).
Axes of the slice: x: 2, y: 2, z: 4, core: 2. Of those that a mesh axis runs over, the one named last changes fastest.
Arguments:
- tokens: bfloat16 [128, 2048], P('ep'), may hold values from -6 to 6
- head_state: float32 [128, 16, 4096], P('ep', 'tp'), may hold values from -6 to 6
- mixer_gain: float32 [2048], replicated, may hold values from 0.1 to 1.9
- w_query: bfloat16 [2048, 1024], P('ep', 'tp'), may hold values from -0.125 to 0.125
- w_key: bfloat16 [2048, 1024], P('ep', 'tp'), may hold values from -0.125 to 0.125
- w_value: bfloat16 [2048, 1024], P('ep', 'tp'), may hold values from -0.125 to 0.125
- decay_down: bfloat16 [2048, 64], replicated, may hold values from -0.125 to 0.125
- decay_up: bfloat16 [64, 1024], replicated, may hold values from -3 to 3
- decay_base: float32 [1024], P('tp'), may hold values from -4 to 0
- rate_down: bfloat16 [2048, 64], replicated, may hold values from -0.125 to 0.125
- rate_up: bfloat16 [64, 1024], replicated, may hold values from -0.75 to 0.75
- head_gain: float32 [1024], P('tp'), may hold values from 0.1 to 1.9
- w_out: bfloat16 [1024, 2048], P('tp', 'ep'), may hold values from -0.1875 to 0.1875
- expert_gain: float32 [2048], replicated, may hold values from 0.1 to 1.9
- expert_ids: int32 [128, 2], P('ep'), may hold values from 0 to 7, all different within a row; in each aligned block of 16 rows (0 to 15, 16 to 31, ...) at most 8 rows name the same one
- route_weight: float32 [128, 2], P('ep'), may hold values from 0.2 to 1
- w_gate: bfloat16 [8, 2048, 512], P('ep', None, 'tp'), may hold values from -0.125 to 0.125
- w_up: bfloat16 [8, 2048, 512], P('ep', None, 'tp'), may hold values from -0.125 to 0.125
- w_down: bfloat16 [8, 512, 2048], P('ep', 'tp'), may hold values from -0.25 to 0.25
Outputs:
- layer_out: bfloat16 [128, 2048], P('ep', 'tp')
- next_state: float32 [128, 16, 4096], P('ep', 'tp')
The draws below stay inside these ranges and needn't reach their ends.
Inputs may be any that keep to these rules, and one draw needn't show every extreme that they name: `expert_ids`: each row names 2 different experts; among the 16 rows of one index of ep no expert is named more than 8 times, and in the rows of some indices one expert is named exactly 8 times.
All inputs are finite; a program needn't handle non-finite values.
Results may differ from the reference program's by a relative error of at most 0.015.
Values may be sent and summed in bfloat16 or wider, within the bound.
A program may use at most 64 MiB of HBM per device.

```python
import math
import jax
import jax.numpy as jnp
import numpy as np
from jax import lax

D = 2048
HEADS = 16
HS = 64
RANK = 64
FF = 512
TOP_K = 2
SEQ_DEV = 16
D_A = 1024
TOKENS = 128
EXPERTS = 8
CAP = 8
N_EP = 8


def level_of(key, dims, pieces, smallest, top_value):
    def one(position, shards_of):
        draws = jax.random.uniform(jax.random.fold_in(jax.random.fold_in(key, 6), position), (shards_of,), jnp.float32, smallest / len(pieces), top_value / len(pieces))
        return jnp.repeat(jnp.exp(draws), dims[position] // shards_of).reshape((-1,) + (1,) * (len(dims) - position - 1))

    level = one(*pieces[0])
    for cut in pieces[1:]:
        level = level * one(*cut)
    return level


def assign_block(stream_key, own, number, rows, count, top, most, lean):
    ranking = jax.random.permutation(stream_key, count)
    packed, ordinary = load_shares(count, rows * top, most, lean, True), load_shares(count, rows * top, most, lean, False)
    places = jnp.arange(count)

    def named(sizes, offset_by):
        used = int((sizes > 0).sum())
        fixed = max(1, used // 4)
        passed = fixed + (places - fixed + offset_by * (used - fixed)) % max(1, count - fixed)
        return jnp.zeros((count,), jnp.int32).at[ranking[jnp.where(places < fixed, places, passed)]].set(jnp.asarray(sizes, jnp.int32))

    sizes = jnp.where(number % 4 == 0, named(packed, number // 4), named(ordinary, number - number // 4 - 1))
    mixed = jax.random.permutation(jax.random.fold_in(own, 3), count)
    giver, receiver = mixed[0:count // 2 * 2:2], mixed[1:count // 2 * 2:2]
    margin = jnp.minimum(sizes[giver] - 1, most - sizes[receiver]) // 2
    margin = jnp.where((giver == ranking[0]) | (receiver == ranking[0]) | (sizes[receiver] == 0), 0, jnp.maximum(margin, 0))
    passed = jax.random.randint(jax.random.fold_in(own, 4), (count // 2,), 0, 1 << 20) % (margin + 1)
    sizes = sizes.at[giver].add(-passed).at[receiver].add(passed)
    labels = jnp.searchsorted(jnp.cumsum(sizes), jnp.arange(rows * top), side="right").astype(jnp.int32)
    listing = labels.reshape(top, rows).T
    listing = listing[jax.random.permutation(jax.random.fold_in(own, 1), rows)]
    offset_by = jax.random.randint(jax.random.fold_in(own, 2), (rows, 1), 0, top)
    return jnp.take_along_axis(listing, (jnp.arange(top)[None, :] + offset_by) % top, axis=1)


def load_shares(amount, total, reach, skew, full):
    weights = [(1 << 20) // math.isqrt(standing ** skew) + 1 for standing in range(1, amount + 1)]
    largest = reach if full else min(reach, max(-(-total // amount), total * weights[0] // sum(weights)))
    least = 1 if total - largest >= amount - 1 else 0
    counts, spare = [largest] + [least] * (amount - 1), total - largest - least * (amount - 1)
    while spare > 0:
        free = [i for i in range(1, amount) if counts[i] < largest] or [i for i in range(1, amount) if counts[i] < reach]
        whole, budget = sum([weights[i] for i in free]), spare
        for i in free:
            addition = min(reach - counts[i], max(1, budget * weights[i] // whole), spare)
            counts[i] = counts[i] + addition
            spare = spare - addition
    return np.array(counts)


def gaussian(stream_key, dims, scale, limit, shards=(), kind=jnp.bfloat16):
    drawn = scale * jax.random.normal(stream_key, dims, jnp.float32)
    if shards:
        drawn = drawn * level_of(stream_key, dims, shards, -0.22, 0.18)
    return jnp.clip(drawn, -limit, limit).astype(kind)


def setup_inputs(seed: int = 0) -> dict:
    splits = jax.random.split(jax.random.key(seed), 20)
    tokens = gaussian(splits[0], (TOKENS, D), 1.0, 6.0, ((0, 8),))
    head_state = gaussian(splits[1], (TOKENS, HEADS, HS * HS), 1.0, 6.0, ((0, 8), (1, 4)), jnp.float32)
    mixer_gain = jnp.clip(1.0 + 0.18 * jax.random.normal(splits[2], (D,), jnp.float32), 0.1, 1.9)
    w_query = gaussian(splits[3], (D, D_A), D ** -0.5, 0.125, ((0, 8), (1, 4)))
    w_key = gaussian(splits[4], (D, D_A), D ** -0.5, 0.125, ((0, 8), (1, 4)))
    w_value = gaussian(splits[5], (D, D_A), D ** -0.5, 0.125, ((0, 8), (1, 4)))
    decay_down = gaussian(splits[6], (D, RANK), D ** -0.5, 0.125)
    decay_up = gaussian(splits[7], (RANK, D_A), 0.5, 3.0)
    decay_base = jnp.clip(-4.0 + 4.0 * jax.random.uniform(splits[8], (D_A,), jnp.float32) ** level_of(splits[8], (D_A,), ((0, 4),), -0.2, 0.2), -4.0, 0.0)
    rate_down = gaussian(splits[9], (D, RANK), D ** -0.5, 0.125)
    rate_up = gaussian(splits[10], (RANK, D_A), RANK ** -0.5, 0.75)
    head_gain = jnp.clip(1.0 + 0.18 * jax.random.normal(splits[11], (D_A,), jnp.float32), 0.1, 1.9)
    w_out = gaussian(splits[12], (D_A, D), D_A ** -0.5, 0.1875, ((0, 4), (1, 8)))
    expert_gain = jnp.clip(1.0 + 0.18 * jax.random.normal(splits[13], (D,), jnp.float32), 0.1, 1.9)
    expert_ids_keys = jax.random.split(jax.random.fold_in(splits[14], 1), TOKENS // SEQ_DEV)
    expert_ids_turns = jax.random.permutation(jax.random.fold_in(splits[14], 3), TOKENS // SEQ_DEV)
    expert_ids = jax.vmap(lambda own, number: assign_block(jax.random.fold_in(splits[14], 2), own, number, SEQ_DEV, EXPERTS, TOP_K, CAP, 2))(expert_ids_keys, expert_ids_turns).reshape((TOKENS, TOP_K))
    route_weight = jnp.clip(jnp.exp(math.log(1.0) - 1.609438 * jax.random.uniform(splits[15], (TOKENS, TOP_K), jnp.float32) ** level_of(splits[15], (TOKENS, TOP_K), ((0, 8),), -0.2, 0.2)), 0.2, 1.0)
    w_gate = gaussian(splits[16], (EXPERTS, D, FF), D ** -0.5, 0.125, ((0, 8), (2, 4)))
    w_up = gaussian(splits[17], (EXPERTS, D, FF), D ** -0.5, 0.125, ((0, 8), (2, 4)))
    w_down = gaussian(splits[18], (EXPERTS, FF, D), FF ** -0.5, 0.25, ((0, 8), (1, 4)))
    return {"tokens": tokens, "head_state": head_state, "mixer_gain": mixer_gain, "w_query": w_query, "w_key": w_key, "w_value": w_value, "decay_down": decay_down, "decay_up": decay_up, "decay_base": decay_base, "rate_down": rate_down, "rate_up": rate_up, "head_gain": head_gain, "w_out": w_out, "expert_gain": expert_gain, "expert_ids": expert_ids, "route_weight": route_weight, "w_gate": w_gate, "w_up": w_up, "w_down": w_down}


norm_eps = 1e-06
group_eps = 0.00064

def rms_scale(activity, gain):
    widened = activity.astype(jnp.float32)
    scaled = widened * lax.rsqrt(lax.optimization_barrier(jnp.mean(widened * widened, axis=-1, keepdims=True)) + norm_eps)
    return (scaled * gain).astype(jnp.bfloat16)

def low_rank(normed, decay_down, decay_up, decay_base, rate_down, rate_up):
    decay_low = jnp.tanh(jnp.dot(normed, decay_down, preferred_element_type=jnp.float32)).astype(jnp.bfloat16)
    decay_pre = decay_base + jnp.dot(decay_low, decay_up, preferred_element_type=jnp.float32)
    decays = jnp.exp(-jnp.exp(-jax.nn.softplus(-decay_pre) - 0.5))
    rate_low = jnp.dot(normed, rate_down, preferred_element_type=jnp.float32).astype(jnp.bfloat16)
    rates = jax.nn.sigmoid(jnp.dot(rate_low, rate_up, preferred_element_type=jnp.float32))
    return (decays, rates)

def recurrence(queries, key_rows, value_rows, decays, rates, old_state, head_gain):
    row_count, head_count, _ = old_state.shape
    head_size = queries.shape[1] // head_count
    head_shape = (row_count, head_count, head_size)
    query_heads = queries.astype(jnp.float32).reshape(head_shape)
    key_heads = key_rows.astype(jnp.float32).reshape(head_shape)
    value_heads = value_rows.astype(jnp.float32).reshape(head_shape)
    decay_heads = decays.reshape(head_shape)
    rate_heads = rates.reshape(head_shape)
    unit_keys = key_heads * lax.rsqrt(lax.optimization_barrier(jnp.sum(key_heads * key_heads, axis=-1, keepdims=True)) + 1.0)
    state_grid = old_state.reshape(row_count, head_count, head_size, head_size)
    removed = lax.optimization_barrier(jnp.sum(state_grid * unit_keys[:, :, None, :], axis=-1))
    updated = state_grid * decay_heads[:, :, None, :] - removed[:, :, :, None] * (unit_keys * rate_heads)[:, :, None, :] + value_heads[:, :, :, None] * key_heads[:, :, None, :]
    readout = lax.optimization_barrier(jnp.sum(updated * query_heads[:, :, None, :], axis=-1))
    centred = readout - lax.optimization_barrier(jnp.mean(readout, axis=-1, keepdims=True))
    spread = lax.optimization_barrier(jnp.mean(centred * centred, axis=-1, keepdims=True))
    scaled = centred * lax.rsqrt(spread + group_eps) * head_gain.reshape(head_count, head_size)
    return (updated.reshape(row_count, head_count, head_size * head_size), scaled.reshape(row_count, head_count * head_size).astype(jnp.bfloat16))

def reference(tokens, head_state, mixer_gain, w_query, w_key, w_value, decay_down, decay_up, decay_base, rate_down, rate_up, head_gain, w_out, expert_gain, expert_ids, route_weight, w_gate, w_up, w_down):
    normed = rms_scale(tokens, mixer_gain)
    queries = jnp.dot(normed, w_query, preferred_element_type=jnp.float32).astype(jnp.bfloat16)
    key_rows = jnp.dot(normed, w_key, preferred_element_type=jnp.float32).astype(jnp.bfloat16)
    value_rows = jnp.dot(normed, w_value, preferred_element_type=jnp.float32).astype(jnp.bfloat16)
    decays, rates = low_rank(normed, decay_down, decay_up, decay_base, rate_down, rate_up)
    next_state, head_out = recurrence(queries, key_rows, value_rows, decays, rates, head_state, head_gain)
    mixed_out = jnp.dot(head_out, w_out, preferred_element_type=jnp.float32)
    residual = (tokens.astype(jnp.float32) + mixed_out).astype(jnp.bfloat16)
    expert_in = rms_scale(residual, expert_gain)
    top_count = expert_ids.shape[1]
    flat_ids = expert_ids.reshape(-1).astype(jnp.int32)
    pair_count = flat_ids.shape[0]
    shares = (route_weight / lax.optimization_barrier(jnp.sum(route_weight, axis=1, keepdims=True))).reshape(-1)
    buffer_rows = N_EP * CAP
    positions = jnp.arange(pair_count, dtype=jnp.int32)

    def one_expert(running, inputs):
        expert, gate_local, up_local, down_local = inputs
        matches = flat_ids == expert
        order_keys = jnp.where(matches, positions, positions + pair_count)
        chosen = jnp.argsort(order_keys)[:buffer_rows].astype(jnp.int32)
        in_range = jnp.arange(buffer_rows, dtype=jnp.int32) < jnp.sum(matches.astype(jnp.int32))
        owners = (chosen // top_count).astype(jnp.int32)
        picked = expert_in[owners]
        gate_act = jnp.dot(picked, gate_local, preferred_element_type=jnp.float32)
        up_act = jnp.dot(picked, up_local, preferred_element_type=jnp.float32)
        hidden = (jax.nn.silu(gate_act) * up_act).astype(jnp.bfloat16)
        result = jnp.dot(hidden, down_local, preferred_element_type=jnp.float32).astype(jnp.bfloat16)
        weights = jnp.where(in_range, shares[chosen], 0.0)
        running = running.at[owners].add(weights[:, None] * result.astype(jnp.float32))
        return (running, None)
    zero_sums = jnp.zeros(expert_in.shape, jnp.float32)
    routed, _ = lax.scan(one_expert, zero_sums, (jnp.arange(EXPERTS, dtype=jnp.int32), w_gate, w_up, w_down))
    layer_out = (residual.astype(jnp.float32) + routed).astype(jnp.bfloat16)
    return (layer_out, next_state)
```

```python
import functools
import math

import jax
import jax.numpy as jnp
from jax import lax
from jax.experimental import pallas as pl
from jax.experimental.pallas import tpu as pltpu
from jax.sharding import PartitionSpec as P

norm_eps = 1e-06
group_eps = 0.00064


def rms_scale(activity, gain):
    widened = activity.astype(jnp.float32)
    scaled = widened * lax.rsqrt(jnp.mean(widened * widened, axis=-1, keepdims=True) + norm_eps)
    return (scaled * gain).astype(jnp.bfloat16)


def low_rank(normed, decay_down, decay_up, decay_base, rate_down, rate_up):
    decay_low = jnp.tanh(jnp.dot(normed, decay_down, preferred_element_type=jnp.float32)).astype(
        jnp.bfloat16
    )
    decay_pre = decay_base + jnp.dot(decay_low, decay_up, preferred_element_type=jnp.float32)
    decays = jnp.exp(-jnp.exp(-jax.nn.softplus(-decay_pre) - 0.5))
    rate_low = jnp.dot(normed, rate_down, preferred_element_type=jnp.float32).astype(jnp.bfloat16)
    rates = jax.nn.sigmoid(jnp.dot(rate_low, rate_up, preferred_element_type=jnp.float32))
    return (decays, rates)


def recurrence(queries, key_rows, value_rows, decays, rates, old_state, head_gain):
    row_count, head_count, _ = old_state.shape
    head_size = queries.shape[1] // head_count
    head_shape = (row_count, head_count, head_size)
    query_heads = queries.astype(jnp.float32).reshape(head_shape)
    key_heads = key_rows.astype(jnp.float32).reshape(head_shape)
    value_heads = value_rows.astype(jnp.float32).reshape(head_shape)
    decay_heads = decays.reshape(head_shape)
    rate_heads = rates.reshape(head_shape)
    unit_keys = key_heads * lax.rsqrt(jnp.sum(key_heads * key_heads, axis=-1, keepdims=True) + 1.0)
    state_grid = old_state.reshape(row_count, head_count, head_size, head_size)
    removed = jnp.sum(state_grid * unit_keys[:, :, None, :], axis=-1)
    updated = (
        state_grid * decay_heads[:, :, None, :]
        - removed[:, :, :, None] * (unit_keys * rate_heads)[:, :, None, :]
        + value_heads[:, :, :, None] * key_heads[:, :, None, :]
    )
    readout = jnp.sum(updated * query_heads[:, :, None, :], axis=-1)
    centred = readout - jnp.mean(readout, axis=-1, keepdims=True)
    spread = jnp.mean(centred * centred, axis=-1, keepdims=True)
    scaled = centred * lax.rsqrt(spread + group_eps) * head_gain.reshape(head_count, head_size)
    return (
        updated.reshape(row_count, head_count, head_size * head_size),
        scaled.reshape(row_count, head_count * head_size).astype(jnp.bfloat16),
    )


def gathered_body(
    tokens,
    head_state,
    mixer_gain,
    w_query,
    w_key,
    w_value,
    decay_down,
    decay_up,
    decay_base,
    rate_down,
    rate_up,
    head_gain,
    w_out,
    expert_gain,
    expert_ids,
    route_weight,
    w_gate,
    w_up,
    w_down,
):
    seq_rows, width = tokens.shape
    local_cols = w_query.shape[1]
    head_lane = lax.axis_index("tp")
    normed = rms_scale(tokens, mixer_gain)
    pieces = (
        lax.all_gather(w_query, "ep", axis=0, tiled=True),
        lax.all_gather(w_key, "ep", axis=0, tiled=True),
        lax.all_gather(w_value, "ep", axis=0, tiled=True),
    )
    projected = tuple(
        (
            jnp.dot(normed, weight_piece, preferred_element_type=jnp.float32)
            for weight_piece in pieces
        )
    )
    queries, key_rows, value_rows = (member.astype(jnp.bfloat16) for member in projected)
    col_offset = head_lane * local_cols
    decays, rates = low_rank(
        normed,
        decay_down,
        lax.dynamic_slice_in_dim(decay_up, col_offset, local_cols, 1),
        decay_base,
        rate_down,
        lax.dynamic_slice_in_dim(rate_up, col_offset, local_cols, 1),
    )
    next_state, head_out = recurrence(
        queries, key_rows, value_rows, decays, rates, head_state, head_gain
    )
    partial_out = jnp.dot(
        head_out,
        lax.all_gather(w_out, "ep", axis=1, tiled=True),
        preferred_element_type=jnp.float32,
    )
    mixed_out = lax.psum(partial_out.astype(jnp.bfloat16), "tp").astype(jnp.float32)
    residual = (tokens.astype(jnp.float32) + mixed_out).astype(jnp.bfloat16)
    expert_in = rms_scale(residual, expert_gain)
    experts = lax.axis_size("ep")
    top_count = expert_ids.shape[1]
    slot_count = max(1, 2 * seq_rows * top_count // experts)
    slot_total = experts * slot_count
    flat_ids = expert_ids.reshape(-1)
    matches = (flat_ids[:, None] == jnp.arange(experts, dtype=jnp.int32)[None, :]).astype(jnp.int32)
    slot_rank = jnp.sum((jnp.cumsum(matches, axis=0) - 1) * matches, axis=1)
    slot_ids = (flat_ids * slot_count + slot_rank).reshape(seq_rows, top_count)
    slot_match = (
        slot_ids[:, :, None] == jnp.arange(slot_total, dtype=jnp.int32)[None, None, :]
    ).astype(jnp.float32)
    picker = jnp.sum(slot_match, axis=1).astype(jnp.bfloat16)
    outbound = jnp.einsum("ts,td->sd", picker, expert_in, preferred_element_type=jnp.float32)
    outbound = outbound.astype(jnp.bfloat16).reshape(experts, slot_count, expert_in.shape[1])
    gate_local, up_local, down_local = (w_gate[0], w_up[0], w_down[0])
    arrived = lax.all_to_all(outbound, "ep", split_axis=0, concat_axis=0, tiled=True)
    sources, held, _ = arrived.shape
    flat_rows = arrived.reshape(sources * held, width)
    gate_act = jnp.dot(flat_rows, gate_local, preferred_element_type=jnp.float32)
    up_act = jnp.dot(flat_rows, up_local, preferred_element_type=jnp.float32)
    hidden = (jax.nn.silu(gate_act) * up_act).astype(jnp.bfloat16)
    partial_rows = jnp.dot(hidden, down_local, preferred_element_type=jnp.float32).reshape(
        sources, held, width
    )
    reduced = lax.psum_scatter(
        partial_rows.astype(jnp.bfloat16), "tp", scatter_dimension=2, tiled=True
    )
    returned = lax.all_to_all(reduced, "ep", split_axis=0, concat_axis=0, tiled=True)
    shares = route_weight / jnp.sum(route_weight, axis=1, keepdims=True)
    combine = jnp.sum(slot_match * shares[:, :, None], axis=1)
    routed = jnp.dot(
        combine,
        returned.reshape(slot_total, -1).astype(jnp.float32),
        precision=lax.Precision.HIGHEST,
    )
    own_cols = routed.shape[1]
    kept = lax.dynamic_slice_in_dim(residual, head_lane * own_cols, own_cols, 1)
    layer_out = (kept.astype(jnp.float32) + routed).astype(jnp.bfloat16)
    return (layer_out, next_state)


f32, bf16 = jnp.float32, jnp.bfloat16


def mm(a, b):
    return jnp.dot(a, b, preferred_element_type=f32)


def split(x):
    top = x.astype(bf16)
    return top, (x - top.astype(f32)).astype(bf16)


def mm_split(x, b):
    top, rest = split(x)
    return mm(top, b) + mm(rest, b)


def ones_where(shape, test):
    rows = lax.broadcasted_iota(jnp.int32, shape, 0)
    cols = lax.broadcasted_iota(jnp.int32, shape, 1)
    return jnp.where(test(rows, cols), 1.0, 0.0).astype(bf16)


def repeat_lanes(x, width):
    return jnp.concatenate([x] * (width // x.shape[1]), axis=1)


def mm_last(a, b):
    return lax.dot_general(a, b, (((1,), (1,)), ((), ())), preferred_element_type=f32)


IN_NAMES = (
    "tok", "ids", "wts", "gain", "ddT", "rdT", "dbase", "dup", "rup", "wq", "wk", "wv",
    "state", "hgain", "wout", "egain", "wg", "wu", "wd",
)


def layer_kernel(n, m, *refs):
    hbm = dict(zip(IN_NAMES, refs))
    refs = refs[len(IN_NAMES) :]
    out, nxt = refs[:2]
    v = dict(zip(IN_NAMES[:-3], refs[2:]))
    refs = refs[2 + len(IN_NAMES) - 3 :]
    (wg2, wu2, wd2, x_r, id_r, q_s, q_r, ho_s, ho_r, p_s, p_r, res_s, own_r, sl_s, sl_r,
     ret_s, ret_r, lsem, w_ss, w_rs, x_ss, x_rs, id_ss, id_rs, q_ss, q_rs, ho_ss, ho_rs, p_ss, p_rs,
     sl_ss, sl_rs, own_ss, own_rs, ret_ss, ret_rs) = refs
    me, lane = lax.axis_index("ep"), lax.axis_index("tp")
    half, core = lane // 2, lax.rem(lane, 2)
    halves = m // 2
    tok, gain = v["tok"], v["gain"]
    B, D = tok.shape
    Ke, C = v["wq"].shape
    heads, wide = v["state"].shape[1:]
    hs = C // heads
    G = n // m
    cap = ret_s.shape[2]
    top = v["ids"].shape[0]
    own_cols = D // m
    F = hbm["wg"].shape[2]

    def remote(src, dst, ss, rs, e, t):
        return pltpu.make_async_remote_copy(
            src_ref=src, dst_ref=dst, send_sem=ss, recv_sem=rs,
            device_id=(e, t), device_id_type=pl.DeviceIdType.MESH,
        )

    barrier = pltpu.get_barrier_semaphore()
    for ke in range(n):
        for kt in range(m):
            if ke or kt:
                pl.semaphore_signal(
                    barrier, inc=1, device_id=(lax.rem(me + ke, n), lax.rem(lane + kt, m)),
                    device_id_type=pl.DeviceIdType.MESH,
                )
    loads = {}
    for i, name in enumerate(IN_NAMES[:-3]):
        loads[name] = pltpu.make_async_copy(hbm[name], v[name], lsem.at[i])
    my_hidden = pl.ds(pl.multiple_of(core * F, F), F)
    spots = (wg2.at[:, my_hidden], wu2.at[:, my_hidden], wd2.at[my_hidden])
    for i, name in enumerate(IN_NAMES[-3:]):
        loads[name] = pltpu.make_async_copy(hbm[name].at[0], spots[i], lsem.at[len(IN_NAMES) - 3 + i])
    for name in IN_NAMES:
        loads[name].start()

    def partner(i, k, count):
        if count & (count - 1):
            return lax.rem(i + k, count)
        for bit in range(count.bit_length() - 1):
            if k >> bit & 1:
                i = i + (1 << bit) * (1 - 2 * (i // (1 << bit) % 2))
        return i

    offsets = list(range(n - 1, 0, -1))
    ep_peers = [(k, partner(me, k, n), lane) for k in offsets]
    tp_peers = [(k, me, lax.rem(lane + k, m)) for k in range(m - 1, 0, -1)]
    slot_peers = [
        ((k, j), partner(me, k, n), lax.rem(lane + 2 * j, m))
        for k in range(n - 1, -1, -1) for j in range(halves - 1, -1, -1) if k or j
    ]
    pending = []

    def send(peers, src_of, dst, ss, rs):
        copies = [remote(src_of(e, t), dst, ss.at[k], rs.at[k], e, t) for k, e, t in peers]
        for c in copies:
            c.start()
        pending.extend(copies)
        return copies

    def arrive(copies):
        for c in copies:
            c.wait_recv()

    def cols_of(ref, index, size):
        return ref[:, pl.ds(pl.multiple_of(index * size, size), size)]

    loads["tok"].wait()
    loads["ids"].wait()
    pl.semaphore_wait(barrier, n * m - 1)
    cx = send(
        ep_peers, lambda e, t: tok.at[:, pl.ds(pl.multiple_of(e * Ke, Ke), Ke)], x_r.at[me], x_ss, x_rs
    )
    cid = send(ep_peers, lambda e, t: v["ids"], id_r.at[me], id_ss, id_rs)
    x_r[me] = cols_of(tok, me, Ke)
    id_r[me] = v["ids"][...]

    for name in IN_NAMES[2:-3]:
        loads[name].wait()
    wide_tok = tok[...].astype(f32)
    scale = lax.rsqrt(jnp.mean(wide_tok * wide_tok, axis=-1, keepdims=True) + norm_eps)
    normed = (wide_tok * scale * gain[...]).astype(bf16)
    decay_low = jnp.tanh(mm_last(normed, v["ddT"][...])).astype(bf16)
    decay_pre = v["dbase"][...] + mm(decay_low, cols_of(v["dup"], lane, C))
    decays = jnp.exp(-(math.exp(-0.5) / (1.0 + jnp.exp(-decay_pre))))
    rate_low = mm_last(normed, v["rdT"][...]).astype(bf16)
    rates = 1.0 / (1.0 + jnp.exp(-mm(rate_low, cols_of(v["rup"], lane, C))))

    R = B * heads
    rep = ones_where((R, B), lambda r, c: r // heads == c)
    rep_t = ones_where((B, R), lambda r, c: c // heads == r)
    head_mask = ones_where((R, C), lambda r, c: c // hs == r % heads).astype(f32)
    fold2 = ones_where((C, 2 * hs), lambda r, c: r % hs == c % hs)
    unfold = ones_where((hs, C), lambda r, c: c % hs == r)
    summing = ones_where((wide, hs), lambda r, c: r // hs == c)
    spreading = ones_where((hs, wide), lambda r, c: c // hs == r)

    def spread(x):
        return mm((mm(rep, x) * head_mask).astype(bf16), fold2)

    def spread_split(x):
        top_part, rest = split(x)
        return spread(top_part) + spread(rest)

    decay_rows = spread_split(decays)
    rate_rows = spread_split(rates)
    gain_rows = spread_split(jnp.broadcast_to(v["hgain"][...], (B, C)))[:, :hs]

    def choice(ids, row_expert, row_slot, same):
        named = functools.reduce(jnp.logical_or, [ids[k : k + 1] == row_expert for k in range(top)])
        hit = jnp.where(jnp.logical_and(named, same), 1.0, 0.0)
        width = hit.shape[1]
        earlier = ones_where((width, width), lambda r, c: jnp.logical_and(r < c, r // B == c // B))
        rank = mm(hit.astype(bf16), earlier)
        return jnp.where(rank == row_slot, hit, 0.0)

    shape = (n * cap, B)
    row = lax.broadcasted_iota(jnp.int32, shape, 0)
    ids = v["ids"][...]
    wts = v["wts"][...]
    shares = wts / jnp.sum(wts, axis=0, keepdims=True)
    share_of = functools.reduce(
        jnp.add, [jnp.where(ids[k : k + 1] == row // cap, shares[k : k + 1], 0.0) for k in range(top)]
    )
    taken = choice(ids, row // cap, (row % cap).astype(f32), row >= 0) * share_of
    eye = ones_where((B, B), lambda r, c: r == c)
    combine = [mm_last(eye, part).astype(bf16) for part in split(taken)]

    arrive(cx)
    rows = x_r[...].reshape(n * B, Ke)
    scaled_rows = (rows.astype(f32) * cols_of(gain, me, Ke)).astype(bf16)
    for i, w in enumerate(("wq", "wk", "wv")):
        q_s[:, :, i * C : (i + 1) * C] = mm(scaled_rows, v[w][...]).astype(bf16).reshape(n, B, C)
    cq = send(ep_peers, lambda e, t: q_s.at[e], q_r.at[me], q_ss, q_rs)
    q_r[me] = q_s[me]

    arrive(cid)
    shape = (n * G * cap, G * B)
    row = lax.broadcasted_iota(jnp.int32, shape, 0)
    col = lax.broadcasted_iota(jnp.int32, shape, 1)
    group_ids = jnp.concatenate([id_r[lane * G + g] for g in range(G)], axis=1)
    picker = choice(
        group_ids, row // (G * cap), (row % cap).astype(f32), row // cap % G == col // B
    ).astype(bf16)

    S = v["state"][...].reshape(R, wide)
    arrive(cq)
    mate = me, half * 2 + (1 - core)
    cw = [
        remote(hbm[name].at[0], spots[i], w_ss.at[i], w_rs.at[i], *mate)
        for i, name in enumerate(IN_NAMES[-3:])
    ]
    for c in cw:
        c.start()
    pending.extend(cw)
    qkv = (jnp.sum(q_r[...].astype(f32), axis=0) * scale).astype(bf16)
    q_rows, k_rows = spread(qkv[:, :C]), spread(qkv[:, C : 2 * C])
    v_rows = spread(qkv[:, 2 * C :])[:, :hs]
    unit = k_rows * lax.rsqrt(jnp.sum(k_rows * k_rows, axis=-1, keepdims=True) * 0.5 + 1.0)
    both = jnp.concatenate(
        [(S * repeat_lanes(x, wide)).astype(bf16) for x in (unit, decay_rows * q_rows)], axis=0
    )
    both = mm(both, summing)
    removed, decayed_read = both[:R], both[R:]
    unit_rates = unit * rate_rows
    unit_read = jnp.sum(unit_rates * q_rows, axis=-1, keepdims=True) * 0.5
    key_read = jnp.sum(k_rows * q_rows, axis=-1, keepdims=True) * 0.5
    readout = decayed_read - removed * unit_read + v_rows * key_read
    centred = readout - jnp.mean(readout, axis=-1, keepdims=True)
    spread_of = jnp.mean(centred * centred, axis=-1, keepdims=True)
    ho_rows = (centred * lax.rsqrt(spread_of + group_eps) * gain_rows).astype(bf16)
    ho = mm(rep_t, (mm(ho_rows, unfold) * head_mask).astype(bf16)).astype(bf16)
    ho_s[...] = ho
    cho = send(ep_peers, lambda e, t: ho_s, ho_r.at[me], ho_ss, ho_rs)
    ho_r[me] = ho
    updated = (
        S * repeat_lanes(decay_rows, wide)
        - mm_split(removed, spreading) * repeat_lanes(unit_rates, wide)
        + mm(v_rows.astype(bf16), spreading) * repeat_lanes(k_rows, wide)
    )
    nxt[...] = updated.reshape(B, heads, wide)

    arrive(cho)
    p_s[...] = mm(ho_r[...].reshape(n * B, C), v["wout"][...]).astype(bf16).reshape(m, G * B, Ke)
    cp = send(tp_peers, lambda e, t: p_s.at[t], p_r.at[lane], p_ss, p_rs)
    p_r[lane] = p_s[lane]
    base = x_r[pl.ds(lane * G, G)].astype(f32).reshape(G * B, Ke)
    arrive(cp)
    res = (base + jnp.sum(p_r[...].astype(f32), axis=0)).astype(bf16)
    sl_s[...] = mm(picker, res).astype(bf16).reshape(n, G * cap, Ke)
    csl = send(slot_peers, lambda e, t: sl_s.at[e], sl_r.at[half, me], sl_ss, sl_rs)
    sl_r[half, me] = sl_s[me]
    res_s[...] = res.reshape(G, B, Ke)
    holder = me // G

    def own_copy(g):
        return remote(
            res_s.at[g], own_r.at[lax.rem(me, G)], own_ss.at[g], own_rs.at[lax.rem(me, G)], lane * G + g, holder
        )

    for g in range(G):
        @pl.when(lane * G + g != me)
        def _():
            own_copy(g).start()

        @pl.when(lane * G + g == me)
        def _():
            own_r[g] = res_s[g]

    for name in IN_NAMES[-3:]:
        loads[name].wait()
    arrive(cw)
    arrive(csl)
    raw = jnp.concatenate(
        [sl_r[:, e].reshape(halves * G * cap, Ke) for e in range(n)], axis=1
    ).astype(f32)
    row_scale = lax.rsqrt(jnp.mean(raw * raw, axis=-1, keepdims=True) + norm_eps)
    xs = (raw * row_scale * v["egain"][...]).astype(bf16)
    gate = mm(xs, wg2[...])
    hidden = (gate / (1.0 + jnp.exp(-gate)) * mm(xs, wu2[...])).astype(bf16)
    y = mm(hidden, wd2[...])
    blocks = [(p, g) for p in range(halves) for g in range(G)]

    def owner(p, g):
        return (2 * p + core) * G + g

    def ret_copy(p, g, t):
        return remote(
            ret_s.at[p * G + g, t], ret_r.at[half, me], ret_ss.at[p * G + g, t], ret_rs.at[half, me],
            owner(p, g), t,
        )

    def not_here(p, g, t):
        return jnp.logical_or(owner(p, g) != me, t != lane)

    for p, g in blocks:
        first = (p * G + g) * cap
        for t in range(m):
            ret_s[p * G + g, t] = y[first : first + cap, t * own_cols : (t + 1) * own_cols].astype(bf16)

            @pl.when(not_here(p, g, t))
            def _():
                ret_copy(p, g, t).start()

        @pl.when(owner(p, g) == me)
        def _():
            ret_r[half, me] = ret_s[p * G + g, lane]

    for g in range(G):
        @pl.when(lane * G + g != me)
        def _():
            remote(res_s.at[g], own_r.at[g], own_ss.at[g], own_rs.at[g], lane * G + g, holder).wait_recv()

    for e in range(n):
        for p in range(halves):
            source = 2 * p + lax.rem(holder, 2)

            @pl.when(jnp.logical_or(e != me, source != lane))
            def _():
                remote(
                    ret_s.at[0, 0], ret_r.at[p, e], ret_ss.at[0, 0], ret_rs.at[p, e], e, source
                ).wait_recv()

    returned = jnp.sum(ret_r[...].astype(f32), axis=0).reshape(n * cap, own_cols).astype(bf16)
    routed = mm(combine[0], returned) + mm(combine[1], returned)
    own = jnp.concatenate([own_r[i] for i in range(G)], axis=1).astype(f32)
    out[...] = (own + routed).astype(bf16)

    for g in range(G):
        @pl.when(lane * G + g != me)
        def _():
            own_copy(g).wait_send()

    for p, g in blocks:
        for t in range(m):
            @pl.when(not_here(p, g, t))
            def _():
                ret_copy(p, g, t).wait_send()

    for c in pending:
        c.wait_send()


def deliver_kernel(small, large, small_out, large_out, sems):
    pieces = sems.shape[0] - 1
    step = large.shape[0] // pieces
    moves = [(small, small_out)] + [
        tuple(ref.at[pl.ds(i * step, step)] for ref in (large, large_out)) for i in range(pieces)
    ]
    writes = [pltpu.make_async_copy(a, b, sems.at[i]) for i, (a, b) in enumerate(moves)]
    for write in writes:
        write.start()
    for write in writes:
        write.wait()


def body(n, m, *args):
    (tokens, head_state, mixer_gain, w_query, w_key, w_value, decay_down, decay_up, decay_base,
     rate_down, rate_up, head_gain, w_out, expert_gain, expert_ids, route_weight, w_gate, w_up, w_down) = args
    B, D = tokens.shape
    Ke, C = w_query.shape
    F = w_gate.shape[2]
    top_count = expert_ids.shape[1]
    cap = max(1, 2 * B * top_count // n)
    if Ke % 128 or C % 128 or F % 128 or (D // m) % 128 or n % m or m % 2 or cap % 8 or B % 16:
        return gathered_body(*args)
    G, own_cols, halves = n // m, D // m, m // 2
    arrays = (
        tokens, expert_ids.T, route_weight.T, mixer_gain[None], decay_down.T, rate_down.T,
        decay_base[None], decay_up, rate_up, w_query, w_key, w_value, head_state,
        head_gain[None], w_out, expert_gain[None], w_gate, w_up, w_down,
    )
    arrays = tuple(pltpu.with_memory_space_constraint(a, pltpu.HBM) for a in arrays)
    V = pltpu.VMEM
    dma = pltpu.SemaphoreType.DMA
    scratch = [V(a.shape, a.dtype) for a in arrays[:-3]] + [
        V((D, 2 * F), bf16), V((D, 2 * F), bf16), V((2 * F, D), bf16),
        V((n, B, Ke), bf16), V((n, top_count, B), jnp.int32),
        V((n, B, 3 * C), bf16), V((n, B, 3 * C), bf16),
        V((B, C), bf16), V((n, B, C), bf16),
        V((m, G * B, Ke), bf16), V((m, G * B, Ke), bf16),
        V((G, B, Ke), bf16), V((G, B, Ke), bf16),
        V((n, G * cap, Ke), bf16), V((halves, n, G * cap, Ke), bf16),
        V((halves * G, m, cap, own_cols), bf16), V((halves, n, cap, own_cols), bf16),
        dma((len(arrays),)), dma((3,)), dma((3,)),
        dma((n,)), dma((n,)), dma((n,)), dma((n,)), dma((n,)), dma((n,)), dma((n,)), dma((n,)),
        dma((m,)), dma((m,)), dma((n, halves)), dma((n, halves)),
        dma((G,)), dma((G,)), dma((halves * G, m)), dma((halves, n)),
    ]
    vm = pl.BlockSpec(memory_space=pltpu.VMEM)
    hbm = pl.BlockSpec(memory_space=pltpu.HBM)
    results = (
        jax.ShapeDtypeStruct((B, own_cols), bf16),
        jax.ShapeDtypeStruct(head_state.shape, f32),
    )
    made = pl.pallas_call(
        functools.partial(layer_kernel, n, m),
        out_shape=tuple(pltpu.VMEM(a.shape, a.dtype) for a in results),
        in_specs=[hbm] * len(arrays),
        out_specs=(vm, vm),
        scratch_shapes=scratch,
        compiler_params=pltpu.CompilerParams(
            collective_id=0, has_side_effects=True, vmem_limit_bytes=32 * 1024 * 1024
        ),
    )(*arrays)
    return pl.pallas_call(
        deliver_kernel,
        out_shape=results,
        in_specs=[vm, vm],
        out_specs=(hbm, hbm),
        scratch_shapes=[dma((1 + math.gcd(B, 4),))],
        compiler_params=pltpu.CompilerParams(vmem_limit_bytes=1024 * 1024),
    )(*made)


def solution(mesh):
    return jax.shard_map(
        functools.partial(body, mesh.shape["ep"], mesh.shape["tp"]),
        mesh=mesh,
        in_specs=(
            P("ep", None),
            P("ep", "tp", None),
            P(),
            P("ep", "tp"),
            P("ep", "tp"),
            P("ep", "tp"),
            P(),
            P(),
            P("tp"),
            P(),
            P(),
            P("tp"),
            P("tp", "ep"),
            P(),
            P("ep", None),
            P("ep", None),
            P("ep", None, "tp"),
            P("ep", None, "tp"),
            P("ep", "tp", None),
        ),
        out_specs=(P("ep", "tp"), P("ep", "tp", None)),
        check_vma=False,
    )
```

```python
import functools
import math

import jax
import jax.numpy as jnp
from jax import lax
from jax.experimental import pallas as pl
from jax.experimental.pallas import tpu as pltpu
from jax.sharding import PartitionSpec as P

norm_eps = 1e-06
group_eps = 0.00064


def rms_scale(activity, gain):
    widened = activity.astype(jnp.float32)
    scaled = widened * lax.rsqrt(jnp.mean(widened * widened, axis=-1, keepdims=True) + norm_eps)
    return (scaled * gain).astype(jnp.bfloat16)


def low_rank(normed, decay_down, decay_up, decay_base, rate_down, rate_up):
    decay_low = jnp.tanh(jnp.dot(normed, decay_down, preferred_element_type=jnp.float32)).astype(
        jnp.bfloat16
    )
    decay_pre = decay_base + jnp.dot(decay_low, decay_up, preferred_element_type=jnp.float32)
    decays = jnp.exp(-jnp.exp(-jax.nn.softplus(-decay_pre) - 0.5))
    rate_low = jnp.dot(normed, rate_down, preferred_element_type=jnp.float32).astype(jnp.bfloat16)
    rates = jax.nn.sigmoid(jnp.dot(rate_low, rate_up, preferred_element_type=jnp.float32))
    return (decays, rates)


def recurrence(queries, key_rows, value_rows, decays, rates, old_state, head_gain):
    row_count, head_count, _ = old_state.shape
    head_size = queries.shape[1] // head_count
    head_shape = (row_count, head_count, head_size)
    query_heads = queries.astype(jnp.float32).reshape(head_shape)
    key_heads = key_rows.astype(jnp.float32).reshape(head_shape)
    value_heads = value_rows.astype(jnp.float32).reshape(head_shape)
    decay_heads = decays.reshape(head_shape)
    rate_heads = rates.reshape(head_shape)
    unit_keys = key_heads * lax.rsqrt(jnp.sum(key_heads * key_heads, axis=-1, keepdims=True) + 1.0)
    state_grid = old_state.reshape(row_count, head_count, head_size, head_size)
    removed = jnp.sum(state_grid * unit_keys[:, :, None, :], axis=-1)
    updated = (
        state_grid * decay_heads[:, :, None, :]
        - removed[:, :, :, None] * (unit_keys * rate_heads)[:, :, None, :]
        + value_heads[:, :, :, None] * key_heads[:, :, None, :]
    )
    readout = jnp.sum(updated * query_heads[:, :, None, :], axis=-1)
    centred = readout - jnp.mean(readout, axis=-1, keepdims=True)
    spread = jnp.mean(centred * centred, axis=-1, keepdims=True)
    scaled = centred * lax.rsqrt(spread + group_eps) * head_gain.reshape(head_count, head_size)
    return (
        updated.reshape(row_count, head_count, head_size * head_size),
        scaled.reshape(row_count, head_count * head_size).astype(jnp.bfloat16),
    )


def gathered_body(
    tokens,
    head_state,
    mixer_gain,
    w_query,
    w_key,
    w_value,
    decay_down,
    decay_up,
    decay_base,
    rate_down,
    rate_up,
    head_gain,
    w_out,
    expert_gain,
    expert_ids,
    route_weight,
    w_gate,
    w_up,
    w_down,
):
    seq_rows, width = tokens.shape
    local_cols = w_query.shape[1]
    head_lane = lax.axis_index("tp")
    normed = rms_scale(tokens, mixer_gain)
    pieces = (
        lax.all_gather(w_query, "ep", axis=0, tiled=True),
        lax.all_gather(w_key, "ep", axis=0, tiled=True),
        lax.all_gather(w_value, "ep", axis=0, tiled=True),
    )
    projected = tuple(
        (
            jnp.dot(normed, weight_piece, preferred_element_type=jnp.float32)
            for weight_piece in pieces
        )
    )
    queries, key_rows, value_rows = (member.astype(jnp.bfloat16) for member in projected)
    col_offset = head_lane * local_cols
    decays, rates = low_rank(
        normed,
        decay_down,
        lax.dynamic_slice_in_dim(decay_up, col_offset, local_cols, 1),
        decay_base,
        rate_down,
        lax.dynamic_slice_in_dim(rate_up, col_offset, local_cols, 1),
    )
    next_state, head_out = recurrence(
        queries, key_rows, value_rows, decays, rates, head_state, head_gain
    )
    partial_out = jnp.dot(
        head_out,
        lax.all_gather(w_out, "ep", axis=1, tiled=True),
        preferred_element_type=jnp.float32,
    )
    mixed_out = lax.psum(partial_out.astype(jnp.bfloat16), "tp").astype(jnp.float32)
    residual = (tokens.astype(jnp.float32) + mixed_out).astype(jnp.bfloat16)
    expert_in = rms_scale(residual, expert_gain)
    experts = lax.axis_size("ep")
    top_count = expert_ids.shape[1]
    slot_count = max(1, 2 * seq_rows * top_count // experts)
    slot_total = experts * slot_count
    flat_ids = expert_ids.reshape(-1)
    matches = (flat_ids[:, None] == jnp.arange(experts, dtype=jnp.int32)[None, :]).astype(jnp.int32)
    slot_rank = jnp.sum((jnp.cumsum(matches, axis=0) - 1) * matches, axis=1)
    slot_ids = (flat_ids * slot_count + slot_rank).reshape(seq_rows, top_count)
    slot_match = (
        slot_ids[:, :, None] == jnp.arange(slot_total, dtype=jnp.int32)[None, None, :]
    ).astype(jnp.float32)
    picker = jnp.sum(slot_match, axis=1).astype(jnp.bfloat16)
    outbound = jnp.einsum("ts,td->sd", picker, expert_in, preferred_element_type=jnp.float32)
    outbound = outbound.astype(jnp.bfloat16).reshape(experts, slot_count, expert_in.shape[1])
    gate_local, up_local, down_local = (w_gate[0], w_up[0], w_down[0])
    arrived = lax.all_to_all(outbound, "ep", split_axis=0, concat_axis=0, tiled=True)
    sources, held, _ = arrived.shape
    flat_rows = arrived.reshape(sources * held, width)
    gate_act = jnp.dot(flat_rows, gate_local, preferred_element_type=jnp.float32)
    up_act = jnp.dot(flat_rows, up_local, preferred_element_type=jnp.float32)
    hidden = (jax.nn.silu(gate_act) * up_act).astype(jnp.bfloat16)
    partial_rows = jnp.dot(hidden, down_local, preferred_element_type=jnp.float32).reshape(
        sources, held, width
    )
    reduced = lax.psum_scatter(
        partial_rows.astype(jnp.bfloat16), "tp", scatter_dimension=2, tiled=True
    )
    returned = lax.all_to_all(reduced, "ep", split_axis=0, concat_axis=0, tiled=True)
    shares = route_weight / jnp.sum(route_weight, axis=1, keepdims=True)
    combine = jnp.sum(slot_match * shares[:, :, None], axis=1)
    routed = jnp.dot(
        combine,
        returned.reshape(slot_total, -1).astype(jnp.float32),
        precision=lax.Precision.HIGHEST,
    )
    own_cols = routed.shape[1]
    kept = lax.dynamic_slice_in_dim(residual, head_lane * own_cols, own_cols, 1)
    layer_out = (kept.astype(jnp.float32) + routed).astype(jnp.bfloat16)
    return (layer_out, next_state)


f32, bf16 = jnp.float32, jnp.bfloat16


def mm(a, b):
    return jnp.dot(a, b, preferred_element_type=f32)


def split(x):
    top = x.astype(bf16)
    return top, (x - top.astype(f32)).astype(bf16)


def mm_split(x, b):
    top, rest = split(x)
    return mm(top, b) + mm(rest, b)


def ones_where(shape, test):
    rows = lax.broadcasted_iota(jnp.int32, shape, 0)
    cols = lax.broadcasted_iota(jnp.int32, shape, 1)
    return jnp.where(test(rows, cols), 1.0, 0.0).astype(bf16)


def repeat_lanes(x, width):
    return jnp.concatenate([x] * (width // x.shape[1]), axis=1)


def mm_last(a, b):
    return lax.dot_general(a, b, (((1,), (1,)), ((), ())), preferred_element_type=f32)


IN_NAMES = (
    "tok", "ids", "wts", "gain", "ddT", "rdT", "dbase", "dup", "rup", "wq", "wk", "wv",
    "state", "hgain", "wout", "egain", "wg", "wu", "wd",
)


VMEM_NAMES = IN_NAMES[:14] + ("egain",)


def layer_kernel(n, m, *refs):
    hbm = dict(zip(IN_NAMES, refs))
    refs = refs[len(IN_NAMES) :]
    out, nxt = refs[:2]
    v = dict(zip(VMEM_NAMES, refs[2:]))
    refs = refs[2 + len(VMEM_NAMES) :]
    (wo, wg2, wu2, wd2, x_r, id_r, q_s, q_r, ho_s, ho_r, res_s, own_r, sl_s, sl_r, ret_s, ret_r,
     lsem, w_ss, w_rs, wo_ss, wo_rs, x_ss, x_rs, id_ss, id_rs, q_ss, q_rs, ho_ss, ho_rs,
     sl_ss, sl_rs, own_ss, own_rs, ret_ss, ret_rs) = refs
    me, lane = lax.axis_index("ep"), lax.axis_index("tp")
    half, core = lane // 2, lax.rem(lane, 2)
    halves = m // 2
    tok, gain = v["tok"], v["gain"]
    B, D = tok.shape
    Ke, C = v["wq"].shape
    heads, wide = v["state"].shape[1:]
    hs = C // heads
    G = n // m
    cap = ret_s.shape[2]
    top = v["ids"].shape[0]
    own_cols = D // m
    F = hbm["wg"].shape[2]
    Q = n // 4

    def lane_of(group):
        return lax.rem(group, halves) * 2 + lax.rem(group, m) // halves

    def group_of(x, c, g):
        return x + halves * c + m * g

    my_groups = [group_of(half, core, g) for g in range(G)]
    my_lane, my_turn = lane_of(me), me // m
    mine = lane == my_lane

    def remote(src, dst, ss, rs, e, t):
        return pltpu.make_async_remote_copy(
            src_ref=src, dst_ref=dst, send_sem=ss, recv_sem=rs,
            device_id=(e, t), device_id_type=pl.DeviceIdType.MESH,
        )

    quarter = me // Q
    low = quarter < 2
    near_q, far_q = jnp.where(low, 2, 1), jnp.where(low, 3, 0)
    own_base = me // (2 * Q) * (2 * Q)
    near = [near_q * Q + lax.rem(me + 1 + i, Q) for i in range(Q)]
    far = [far_q * Q + lax.rem(me + 1 + i, Q) for i in range(Q)]
    close = [own_base + lax.rem(me + k, 2 * Q) for k in range(2 * Q - 1, 0, -1)]
    ep_peers = far + near + close
    tp_peers = [lax.rem(lane + k, m) for k in range(m - 1, 0, -1)]

    loads = {}
    spots = {name: v[name] for name in VMEM_NAMES}
    my_hidden = pl.ds(pl.multiple_of(core * F, F), F)
    spots["wout"] = wo.at[lane]
    spots["wg"], spots["wu"], spots["wd"] = wg2.at[:, my_hidden], wu2.at[:, my_hidden], wd2.at[my_hidden]
    for i, name in enumerate(IN_NAMES):
        src = hbm[name]
        if name in ("dup", "rup"):
            src = src.at[:, pl.ds(pl.multiple_of(lane * C, C), C)]
        elif name in ("wg", "wu", "wd"):
            src = src.at[0]
        loads[name] = pltpu.make_async_copy(src, spots[name], lsem.at[i])
    loads["tok"].start()
    barrier = pltpu.get_barrier_semaphore()
    for e, t in [(e, lane) for e in ep_peers] + [(me, t) for t in tp_peers]:
        pl.semaphore_signal(barrier, inc=1, device_id=(e, t), device_id_type=pl.DeviceIdType.MESH)
    for name in IN_NAMES[1:]:
        loads[name].start()

    pending = []

    def start(*copies):
        for c in copies:
            c.start()
        pending.extend(copies)

    def cols_of(ref, index, size):
        return ref[:, pl.ds(pl.multiple_of(index * size, size), size)]

    loads["tok"].wait()
    pl.semaphore_wait(barrier, n + m - 2)
    for i, e in enumerate(ep_peers):
        start(remote(
            tok.at[:, pl.ds(pl.multiple_of(e * Ke, Ke), Ke)], x_r.at[me], x_ss.at[i], x_rs.at[me], e, lane
        ))
    for i, t in enumerate(tp_peers):
        start(remote(hbm["wout"], wo.at[lane], wo_ss.at[i], wo_rs.at[lane], me, t))
    mate = me, half * 2 + (1 - core)
    cw = [
        remote(hbm[name].at[0], spots[name], w_ss.at[i], w_rs.at[i], *mate)
        for i, name in enumerate(IN_NAMES[-3:])
    ]
    start(*cw)
    x_r[me] = cols_of(tok, me, Ke)
    loads["ids"].wait()
    id_copies = [remote(v["ids"], id_r.at[my_turn], id_ss.at[i], id_rs.at[my_turn], e, lane) for i, e in enumerate(ep_peers)]

    @pl.when(mine)
    def _():
        for c in id_copies:
            c.start()
        id_r[my_turn] = v["ids"][...]

    for name in IN_NAMES[2:]:
        if name not in ("wout", "wg", "wu", "wd"):
            loads[name].wait()
    wide_tok = tok[...].astype(f32)
    scale = lax.rsqrt(jnp.mean(wide_tok * wide_tok, axis=-1, keepdims=True) + norm_eps)
    normed = (wide_tok * scale * gain[...]).astype(bf16)
    decay_low = jnp.tanh(mm_last(normed, v["ddT"][...])).astype(bf16)
    decay_pre = v["dbase"][...] + mm(decay_low, v["dup"][...])
    decays = jnp.exp(-(math.exp(-0.5) / (1.0 + jnp.exp(-decay_pre))))
    rate_low = mm_last(normed, v["rdT"][...]).astype(bf16)
    rates = 1.0 / (1.0 + jnp.exp(-mm(rate_low, v["rup"][...])))

    R = B * heads
    rep = ones_where((R, B), lambda r, c: r // heads == c)
    rep_t = ones_where((B, R), lambda r, c: c // heads == r)
    head_mask = ones_where((R, C), lambda r, c: c // hs == r % heads).astype(f32)
    fold2 = ones_where((C, 2 * hs), lambda r, c: r % hs == c % hs)
    unfold = ones_where((hs, C), lambda r, c: c % hs == r)
    summing = ones_where((wide, hs), lambda r, c: r // hs == c)
    spreading = ones_where((hs, wide), lambda r, c: c // hs == r)

    def spread(x):
        return mm((mm(rep, x) * head_mask).astype(bf16), fold2)

    def spread_split(x):
        top_part, rest = split(x)
        return spread(top_part) + spread(rest)

    decay_rows = spread_split(decays)
    rate_rows = spread_split(rates)
    gain_rows = spread_split(jnp.broadcast_to(v["hgain"][...], (B, C)))[:, :hs]

    def project(first, count, peers):
        for e in peers:
            remote(x_r.at[e], x_r.at[e], x_ss.at[0], x_rs.at[e], e, lane).wait_recv()
        block = pl.ds(pl.multiple_of(first, count), count)
        rows = x_r[block].reshape(count * B, Ke)
        scaled_rows = (rows.astype(f32) * cols_of(gain, me, Ke)).astype(bf16)
        for i, w in enumerate(("wq", "wk", "wv")):
            q_s[block, :, i * C : (i + 1) * C] = mm(scaled_rows, v[w][...]).astype(bf16).reshape(count, B, C)
        for e in peers:
            start(remote(q_s.at[e], q_r.at[me], q_ss.at[e], q_rs.at[me], e, lane))

    project(near_q * Q, Q, near)
    project(own_base, 2 * Q, close)
    project(far_q * Q, Q, far)
    q_r[me] = q_s[me]

    def choice(ids, row_expert, row_slot, same):
        named = functools.reduce(jnp.logical_or, [ids[k : k + 1] == row_expert for k in range(top)])
        hit = jnp.where(jnp.logical_and(named, same), 1.0, 0.0)
        width = hit.shape[1]
        earlier = ones_where((width, width), lambda r, c: jnp.logical_and(r < c, r // B == c // B))
        rank = mm(hit.astype(bf16), earlier)
        return jnp.where(rank == row_slot, hit, 0.0)

    shape = (n * cap, B)
    row = lax.broadcasted_iota(jnp.int32, shape, 0)
    ids = v["ids"][...]
    wts = v["wts"][...]
    shares = wts / jnp.sum(wts, axis=0, keepdims=True)
    share_of = functools.reduce(
        jnp.add, [jnp.where(ids[k : k + 1] == row // cap, shares[k : k + 1], 0.0) for k in range(top)]
    )
    taken = choice(ids, row // cap, (row % cap).astype(f32), row >= 0) * share_of
    eye = ones_where((B, B), lambda r, c: r == c)
    combine = [mm_last(eye, part).astype(bf16) for part in split(taken)]

    for g in range(G):
        @pl.when(my_groups[g] != me)
        def _():
            remote(id_r.at[g], id_r.at[g], id_ss.at[0], id_rs.at[g], my_groups[g], lane).wait_recv()

    shape = (n * G * cap, G * B)
    row = lax.broadcasted_iota(jnp.int32, shape, 0)
    col = lax.broadcasted_iota(jnp.int32, shape, 1)
    group_ids = jnp.concatenate([id_r[g] for g in range(G)], axis=1)
    picker = choice(
        group_ids, row // (G * cap), (row % cap).astype(f32), row // cap % G == col // B
    ).astype(bf16)
    base = jnp.concatenate([x_r[my_groups[g]] for g in range(G)], axis=0).astype(f32)

    S = v["state"][...].reshape(R, wide)
    for e in close + near + far:
        remote(q_r.at[e], q_r.at[e], q_ss.at[0], q_rs.at[e], e, lane).wait_recv()
    qkv = (jnp.sum(q_r[...].astype(f32), axis=0) * scale).astype(bf16)
    q_rows, k_rows = spread(qkv[:, :C]), spread(qkv[:, C : 2 * C])
    v_rows = spread(qkv[:, 2 * C :])[:, :hs]
    unit = k_rows * lax.rsqrt(jnp.sum(k_rows * k_rows, axis=-1, keepdims=True) * 0.5 + 1.0)
    both = jnp.concatenate(
        [(S * repeat_lanes(x, wide)).astype(bf16) for x in (unit, decay_rows * q_rows)], axis=0
    )
    both = mm(both, summing)
    removed, decayed_read = both[:R], both[R:]
    unit_rates = unit * rate_rows
    unit_read = jnp.sum(unit_rates * q_rows, axis=-1, keepdims=True) * 0.5
    key_read = jnp.sum(k_rows * q_rows, axis=-1, keepdims=True) * 0.5
    readout = decayed_read - removed * unit_read + v_rows * key_read
    centred = readout - jnp.mean(readout, axis=-1, keepdims=True)
    spread_of = jnp.mean(centred * centred, axis=-1, keepdims=True)
    ho_rows = (centred * lax.rsqrt(spread_of + group_eps) * gain_rows).astype(bf16)
    ho = mm(rep_t, (mm(ho_rows, unfold) * head_mask).astype(bf16)).astype(bf16)
    ho_s[...] = ho

    def ho_copy(e, i):
        return remote(ho_s, ho_r.at[my_turn, lane], ho_ss.at[i], ho_rs.at[my_turn, lane], e, my_lane)

    start(*[ho_copy(e, i) for i, e in enumerate(ep_peers)])

    @pl.when(jnp.logical_not(mine))
    def _():
        ho_copy(me, n - 1).start()

    @pl.when(mine)
    def _():
        ho_r[my_turn, lane] = ho_s[...]

    updated = (
        S * repeat_lanes(decay_rows, wide)
        - mm_split(removed, spreading) * repeat_lanes(unit_rates, wide)
        + mm(v_rows.astype(bf16), spreading) * repeat_lanes(k_rows, wide)
    )
    nxt[...] = updated.reshape(B, heads, wide)
    loads["wout"].wait()
    for t in tp_peers:
        remote(wo.at[t], wo.at[t], wo_ss.at[0], wo_rs.at[t], me, t).wait_recv()

    for g in range(G):
        for t in range(m):
            @pl.when(jnp.logical_or(my_groups[g] != me, t != lane))
            def _():
                remote(ho_r.at[g, t], ho_r.at[g, t], ho_ss.at[0], ho_rs.at[g, t], my_groups[g], t).wait_recv()

    mixed = functools.reduce(jnp.add, [mm(ho_r[:, t].reshape(G * B, C), wo[t]) for t in range(m)])
    res = (base + mixed).astype(bf16)
    sl_s[...] = mm(picker, res).astype(bf16).reshape(n, G * cap, Ke)
    slot_peers = [(e, lax.rem(lane + 2 * j, m)) for j in range(halves - 1, -1, -1) for e in ep_peers]
    slot_peers += [(me, lax.rem(lane + 2 * j, m)) for j in range(halves - 1, 0, -1)]
    start(*[
        remote(sl_s.at[e], sl_r.at[half, me], sl_ss.at[i], sl_rs.at[half, me], e, t)
        for i, (e, t) in enumerate(slot_peers)
    ])
    sl_r[half, me] = sl_s[me]
    res_s[...] = res.reshape(G, B, Ke)
    holder, place = me // G, lax.rem(me, G)

    def own_copy(g):
        return remote(
            res_s.at[g], own_r.at[place], own_ss.at[g], own_rs.at[place], my_groups[g], holder
        )

    def own_here(g):
        return jnp.logical_and(my_groups[g] == me, holder == lane)

    for g in range(G):
        @pl.when(jnp.logical_not(own_here(g)))
        def _():
            own_copy(g).start()

        @pl.when(own_here(g))
        def _():
            own_r[place] = res_s[g]

    for name in IN_NAMES[-3:]:
        loads[name].wait()
    for c in cw:
        c.wait_recv()

    def slots_in(first, count, sources):
        for p in range(halves):
            for e in sources:
                remote(sl_r.at[p, e], sl_r.at[p, e], sl_ss.at[0], sl_rs.at[p, e], e, 2 * p + core).wait_recv()
        if sources is close:
            for j in range(1, halves):
                p = lax.rem(half + j, halves)
                remote(sl_r.at[p, me], sl_r.at[p, me], sl_ss.at[0], sl_rs.at[p, me], me, 2 * p + core).wait_recv()
        raw = jnp.concatenate(
            [sl_r[:, first + e].reshape(halves * G * cap, Ke) for e in range(count)], axis=1
        ).astype(f32)
        block = pl.ds(pl.multiple_of(first * Ke, Ke), count * Ke)
        xs = (raw * v["egain"][:, block]).astype(bf16)
        return jnp.sum(raw * raw, axis=-1, keepdims=True), mm(xs, wg2[block]), mm(xs, wu2[block])

    parts = [slots_in(own_base, 2 * Q, close)]
    parts.append(slots_in(near_q * Q, Q, near))
    parts.append(slots_in(far_q * Q, Q, far))
    square, gate, up = (functools.reduce(jnp.add, terms) for terms in zip(*parts))
    row_scale = lax.rsqrt(square / D + norm_eps)
    gate = gate * row_scale
    hidden = (gate / (1.0 + jnp.exp(-gate)) * (up * row_scale)).astype(bf16)
    y = mm(hidden, wd2[...])
    blocks = [(p, g) for p in range(halves) for g in range(G)]

    def ret_copy(p, g, t):
        return remote(
            ret_s.at[p * G + g, t], ret_r.at[half, me], ret_ss.at[p * G + g, t], ret_rs.at[half, me],
            group_of(p, core, g), t,
        )

    def not_here(p, g, t):
        return jnp.logical_or(group_of(p, core, g) != me, t != lane)

    for p, g in blocks:
        first = (p * G + g) * cap
        for t in range(m):
            ret_s[p * G + g, t] = y[first : first + cap, t * own_cols : (t + 1) * own_cols].astype(bf16)

            @pl.when(not_here(p, g, t))
            def _():
                ret_copy(p, g, t).start()

        @pl.when(group_of(p, core, g) == me)
        def _():
            ret_r[half, me] = ret_s[p * G + g, lane]

    for i in range(G):
        source = lane * G + i

        @pl.when(jnp.logical_not(jnp.logical_and(source == me, mine)))
        def _():
            remote(own_r.at[i], own_r.at[i], own_ss.at[0], own_rs.at[i], source, my_lane).wait_recv()

    for e in range(n):
        for p in range(halves):
            source = 2 * p + lax.rem(my_lane, 2)

            @pl.when(jnp.logical_or(e != me, source != lane))
            def _():
                remote(
                    ret_s.at[0, 0], ret_r.at[p, e], ret_ss.at[0, 0], ret_rs.at[p, e], e, source
                ).wait_recv()

    returned = jnp.sum(ret_r[...].astype(f32), axis=0).reshape(n * cap, own_cols).astype(bf16)
    routed = mm(combine[0], returned) + mm(combine[1], returned)
    own = jnp.concatenate([own_r[i] for i in range(G)], axis=1).astype(f32)
    out[...] = (own + routed).astype(bf16)

    @pl.when(mine)
    def _():
        for c in id_copies:
            c.wait_send()

    @pl.when(jnp.logical_not(mine))
    def _():
        ho_copy(me, n - 1).wait_send()

    for g in range(G):
        @pl.when(jnp.logical_not(own_here(g)))
        def _():
            own_copy(g).wait_send()

    for p, g in blocks:
        for t in range(m):
            @pl.when(not_here(p, g, t))
            def _():
                ret_copy(p, g, t).wait_send()

    for c in pending:
        c.wait_send()


def deliver_kernel(small, large, small_out, large_out, sems):
    pieces = sems.shape[0] - 1
    step = large.shape[0] // pieces
    moves = [(small, small_out)] + [
        tuple(ref.at[pl.ds(i * step, step)] for ref in (large, large_out)) for i in range(pieces)
    ]
    writes = [pltpu.make_async_copy(a, b, sems.at[i]) for i, (a, b) in enumerate(moves)]
    for write in writes:
        write.start()
    for write in writes:
        write.wait()


def body(n, m, *args):
    (tokens, head_state, mixer_gain, w_query, w_key, w_value, decay_down, decay_up, decay_base,
     rate_down, rate_up, head_gain, w_out, expert_gain, expert_ids, route_weight, w_gate, w_up, w_down) = args
    B, D = tokens.shape
    Ke, C = w_query.shape
    F = w_gate.shape[2]
    top_count = expert_ids.shape[1]
    cap = max(1, 2 * B * top_count // n)
    if Ke % 128 or C % 128 or F % 128 or (D // m) % 128 or n % m or n % 4 or m % 2 or cap % 8 or B % 16:
        return gathered_body(*args)
    G, own_cols, halves = n // m, D // m, m // 2
    arrays = (
        tokens, expert_ids.T, route_weight.T, mixer_gain[None], decay_down.T, rate_down.T,
        decay_base[None], decay_up, rate_up, w_query, w_key, w_value, head_state,
        head_gain[None], w_out, expert_gain[None], w_gate, w_up, w_down,
    )
    arrays = tuple(pltpu.with_memory_space_constraint(a, pltpu.HBM) for a in arrays)
    V = pltpu.VMEM
    dma = pltpu.SemaphoreType.DMA
    shapes = {name: a.shape for name, a in zip(IN_NAMES, arrays)}
    shapes["dup"] = shapes["rup"] = (decay_up.shape[0], C)
    kinds = {name: a.dtype for name, a in zip(IN_NAMES, arrays)}
    scratch = [V(shapes[name], kinds[name]) for name in VMEM_NAMES] + [
        V((m, C, Ke), bf16), V((D, 2 * F), bf16), V((D, 2 * F), bf16), V((2 * F, D), bf16),
        V((n, B, Ke), bf16), V((G, top_count, B), jnp.int32),
        V((n, B, 3 * C), bf16), V((n, B, 3 * C), bf16),
        V((B, C), bf16), V((G, m, B, C), bf16),
        V((G, B, Ke), bf16), V((G, B, Ke), bf16),
        V((n, G * cap, Ke), bf16), V((halves, n, G * cap, Ke), bf16),
        V((halves * G, m, cap, own_cols), bf16), V((halves, n, cap, own_cols), bf16),
        dma((len(arrays),)), dma((3,)), dma((3,)), dma((m,)), dma((m,)),
        dma((n,)), dma((n,)), dma((n,)), dma((G,)), dma((n,)), dma((n,)), dma((n,)), dma((G, m)),
        dma((n * halves,)), dma((halves, n)),
        dma((G,)), dma((G,)), dma((halves * G, m)), dma((halves, n)),
    ]
    vm = pl.BlockSpec(memory_space=pltpu.VMEM)
    hbm = pl.BlockSpec(memory_space=pltpu.HBM)
    results = (
        jax.ShapeDtypeStruct((B, own_cols), bf16),
        jax.ShapeDtypeStruct(head_state.shape, f32),
    )
    made = pl.pallas_call(
        functools.partial(layer_kernel, n, m),
        out_shape=tuple(pltpu.VMEM(a.shape, a.dtype) for a in results),
        in_specs=[hbm] * len(arrays),
        out_specs=(vm, vm),
        scratch_shapes=scratch,
        compiler_params=pltpu.CompilerParams(
            collective_id=0, has_side_effects=True, vmem_limit_bytes=32 * 1024 * 1024
        ),
    )(*arrays)
    return pl.pallas_call(
        deliver_kernel,
        out_shape=results,
        in_specs=[vm, vm],
        out_specs=(hbm, hbm),
        scratch_shapes=[dma((1 + math.gcd(B, 4),))],
        compiler_params=pltpu.CompilerParams(vmem_limit_bytes=1024 * 1024),
    )(*made)


def solution(mesh):
    return jax.shard_map(
        functools.partial(body, mesh.shape["ep"], mesh.shape["tp"]),
        mesh=mesh,
        in_specs=(
            P("ep", None),
            P("ep", "tp", None),
            P(),
            P("ep", "tp"),
            P("ep", "tp"),
            P("ep", "tp"),
            P(),
            P(),
            P("tp"),
            P(),
            P(),
            P("tp"),
            P("tp", "ep"),
            P(),
            P("ep", None),
            P("ep", None),
            P("ep", None, "tp"),
            P("ep", None, "tp"),
            P("ep", "tp", None),
        ),
        out_specs=(P("ep", "tp"), P("ep", "tp", None)),
        check_vma=False,
    )
```
